32 devices in a mesh: grp: 2 (over y), fs: 4 (over z), tp: 4 (over x, core).
Axes of the slice: x: 2, y: 2, z: 4, core: 2. Of those that a mesh axis runs over, the one named last changes fastest.
Arguments:
- tokens: bfloat16 [8192, 2048], P(('grp', 'fs'), 'tp'), parts along dimension 0, may hold values from -6 to 6
- norm1_gain: float32 [2048], replicated, may hold values from 0.1 to 1.9
- weight_u: float32 [2048, 1024], P('fs', 'tp'), may hold values from -0.125 to 0.125
- weight_v: float32 [2048, 1024], P('fs', 'tp'), may hold values from -0.125 to 0.125
- scale_u: float32 [1024], P('tp'), may hold values from 0.5 to 2
- scale_v: float32 [1024], P('tp'), may hold values from 0.05 to 4.5
- mix_gain: float32 [1024], P('tp'), may hold values from 0.1 to 1.9
- spatial_weight: float32 [4, 128, 128], replicated, may hold values from -0.5 to 0.5
- spatial_bias: float32 [4, 128], replicated, may hold values from 0.5 to 1.5
- weight_out: float32 [1024, 2048], P('tp', 'fs'), may hold values from -0.1875 to 0.1875
- scale_out: float32 [2048], P('fs'), may hold values from 0.5 to 2
- norm2_gain: float32 [2048], replicated, may hold values from 0.1 to 1.9
- weight_up: float32 [2048, 8192], P('fs', 'tp'), may hold values from -0.125 to 0.125
- scale_up: float32 [8192], P('tp'), may hold values from 0.5 to 2
- weight_down: float32 [8192, 2048], P('tp', 'fs'), may hold values from -0.0625 to 0.0625
- scale_down: float32 [2048], P('fs'), may hold values from 0.5 to 2
Outputs:
- result: bfloat16 [8192, 2048], P(('grp', 'fs'), 'tp'), parts along dimension 0
The draws below stay inside these ranges and needn't reach their ends.
There are 2 independent parts, one for each index of `grp`. The reference program is written for one: setup_inputs(seed, part) draws one part's arguments, and reference() takes and returns one part's arrays. A program takes and returns all parts, laid end to end along the dimension named above; an argument that names none is the same for every part. Nothing has to cross between parts.
All inputs are finite; a program needn't handle non-finite values.
Results may differ from the reference program's by a relative error of at most 0.023.
Values may be sent and summed in bfloat16 or wider, within the bound.
No kernel may reach another device: no remote copies, remote signals or barrier semaphores. Data moves between devices by JAX's collectives and lax.ppermute only.
A program may use at most 128 MiB of HBM per device.

```python
import math
import jax
import jax.numpy as jnp
from jax import lax

D = 2048
GM_W = 1024
GROUPS = 4
BLOCK = 128
FF = 8192
TOKENS = 4096
N_TP = 4


def draw_scale_v(key, part):
    columns = jnp.arange(GM_W, dtype=jnp.float32) / GM_W
    roughness = jax.random.uniform(key, (GM_W,), jnp.float32, 0.5, 1.5)
    return 0.4 * jnp.exp(columns * jnp.log(4.0)) * roughness


def level_of(stream_key, dims, split, least, top_value):
    gain, own = 1.0, jax.random.fold_in(stream_key, 6)
    for axis_at, blocks in split:
        heights = jnp.exp(jax.random.uniform(jax.random.fold_in(own, axis_at), (blocks,), jnp.float32, least / len(split), top_value / len(split)))
        gain = gain * jnp.repeat(heights, dims[axis_at] // blocks).reshape([-1 if axis == axis_at else 1 for axis in range(len(dims))])
    return gain


def bell_draw(stream_key, dims, spread, limit, cuts=(), kind=jnp.bfloat16):
    entries = spread * jax.random.normal(stream_key, dims, jnp.float32)
    if cuts:
        entries = entries * level_of(stream_key, dims, cuts, -0.22, 0.18)
    return jnp.clip(entries, -limit, limit).astype(kind)


def setup_inputs(seed: int = 0, part: int = 0) -> dict:
    seeds = jax.random.split(jax.random.key(seed), 17)
    part_keys = jax.random.split(jax.random.fold_in(seeds[16], part), 17)
    tokens = bell_draw(part_keys[0], (TOKENS, D), 1.0, 6.0, ((0, 4), (1, 4)))
    norm1_gain = jnp.clip(1.0 + 0.18 * jax.random.normal(seeds[1], (D,), jnp.float32), 0.1, 1.9)
    weight_u = bell_draw(seeds[2], (D, GM_W), D ** -0.5, 0.125, ((0, 4), (1, 4)), jnp.float32)
    weight_v = bell_draw(seeds[3], (D, GM_W), D ** -0.5, 0.125, ((0, 4), (1, 4)), jnp.float32)
    scale_u = jnp.clip(jnp.exp(math.log(2.0) - 1.3862944 * jax.random.uniform(seeds[4], (GM_W,), jnp.float32) ** level_of(seeds[4], (GM_W,), ((0, 4),), -0.2, 0.2)), 0.5, 2.0)
    scale_v = draw_scale_v(jax.random.fold_in(seeds[16], 71), part)
    mix_gain = jnp.clip(1.0 + 0.18 * jax.random.normal(seeds[6], (GM_W,), jnp.float32), 0.1, 1.9)
    spatial_weight = bell_draw(seeds[7], (GROUPS, BLOCK, BLOCK), BLOCK ** -0.5, 0.5, (), jnp.float32)
    spatial_bias = jnp.clip(jax.random.uniform(seeds[8], (GROUPS, BLOCK), jnp.float32, 0.5, 1.5), 0.5, 1.5)
    weight_out = bell_draw(seeds[9], (GM_W, D), GM_W ** -0.5, 0.1875, ((0, 4), (1, 4)), jnp.float32)
    scale_out = jnp.clip(jnp.exp(math.log(2.0) - 1.3862944 * jax.random.uniform(seeds[10], (D,), jnp.float32) ** level_of(seeds[10], (D,), ((0, 4),), -0.2, 0.2)), 0.5, 2.0)
    norm2_gain = jnp.clip(1.0 + 0.18 * jax.random.normal(seeds[11], (D,), jnp.float32), 0.1, 1.9)
    weight_up = bell_draw(seeds[12], (D, FF), D ** -0.5, 0.125, ((0, 4), (1, 4)), jnp.float32)
    scale_up = jnp.clip(jnp.exp(math.log(2.0) - 1.3862944 * jax.random.uniform(seeds[13], (FF,), jnp.float32) ** level_of(seeds[13], (FF,), ((0, 4),), -0.2, 0.2)), 0.5, 2.0)
    weight_down = bell_draw(seeds[14], (FF, D), FF ** -0.5, 0.0625, ((0, 4), (1, 4)), jnp.float32)
    scale_down = jnp.clip(jnp.exp(math.log(2.0) - 1.3862944 * jax.random.uniform(seeds[15], (D,), jnp.float32) ** level_of(seeds[15], (D,), ((0, 4),), -0.2, 0.2)), 0.5, 2.0)
    return {"tokens": tokens, "norm1_gain": norm1_gain, "weight_u": weight_u, "weight_v": weight_v, "scale_u": scale_u, "scale_v": scale_v, "mix_gain": mix_gain, "spatial_weight": spatial_weight, "spatial_bias": spatial_bias, "weight_out": weight_out, "scale_out": scale_out, "norm2_gain": norm2_gain, "weight_up": weight_up, "scale_up": scale_up, "weight_down": weight_down, "scale_down": scale_down}


def rms_rows(values, gain_vector):
    widened = values.astype(jnp.float32)
    scaled = widened * lax.rsqrt(lax.optimization_barrier(jnp.mean(widened * widened, axis=-1, keepdims=True)) + 1e-06)
    return (scaled * gain_vector).astype(jnp.bfloat16)

def run_sum(operand_left, operand_right, column_scale, pieces):
    run_width = operand_left.shape[1] // pieces
    running = jnp.zeros((operand_left.shape[0], operand_right.shape[1]), jnp.float32)
    for run_index in range(pieces):
        lower = run_index * run_width
        partial_term = jnp.dot(operand_left[:, lower:lower + run_width], operand_right[lower:lower + run_width], preferred_element_type=jnp.float32) * column_scale
        running = running + lax.optimization_barrier(partial_term.astype(jnp.bfloat16)).astype(jnp.float32)
    return running

def reference(tokens, norm1_gain, weight_u, weight_v, scale_u, scale_v, mix_gain, spatial_weight, spatial_bias, weight_out, scale_out, norm2_gain, weight_up, scale_up, weight_down, scale_down):
    normed_in = rms_rows(tokens, norm1_gain)
    pre_u = jnp.dot(normed_in, weight_u.astype(jnp.bfloat16), preferred_element_type=jnp.float32) * scale_u
    pre_v = jnp.dot(normed_in, weight_v.astype(jnp.bfloat16), preferred_element_type=jnp.float32) * scale_v
    gate_u = jax.nn.gelu(pre_u)
    act_v = jax.nn.gelu(pre_v)
    row_mean = lax.optimization_barrier(jnp.mean(act_v, axis=-1, keepdims=True))
    square = lax.optimization_barrier(jnp.mean(act_v * act_v, axis=-1, keepdims=True))
    v_norm = ((act_v - row_mean) * lax.rsqrt(square - row_mean * row_mean + 1e-06) * mix_gain).astype(jnp.bfloat16)
    lower_mask = jnp.tril(jnp.ones((BLOCK, BLOCK), jnp.float32))
    spatial_mask = (spatial_weight * lower_mask).astype(jnp.bfloat16)
    blocks = v_norm.reshape(TOKENS // BLOCK, BLOCK, GROUPS, GM_W // GROUPS)
    mixed_cols = jnp.einsum('gts,nsgc->ntgc', spatial_mask.astype(jnp.float32), blocks.astype(jnp.float32))
    mixed_cols = mixed_cols + spatial_bias.T[None, :, :, None]
    gated = (gate_u * mixed_cols.reshape(TOKENS, GM_W)).astype(jnp.bfloat16)
    mixer_sum = run_sum(gated, weight_out.astype(jnp.bfloat16), scale_out, N_TP)
    residual = (tokens.astype(jnp.float32) + mixer_sum).astype(jnp.bfloat16)
    normed_mid = rms_rows(residual, norm2_gain)
    pre_up = jnp.dot(normed_mid, weight_up.astype(jnp.bfloat16), preferred_element_type=jnp.float32) * scale_up
    hidden = jnp.square(jax.nn.relu(pre_up)).astype(jnp.bfloat16)
    channel_sum = run_sum(hidden, weight_down.astype(jnp.bfloat16), scale_down, N_TP)
    return (residual.astype(jnp.float32) + channel_sum).astype(jnp.bfloat16)
```

```python
import jax
import jax.numpy as jnp
from jax import lax
from jax.sharding import PartitionSpec as P

GM_W = 1024
GROUPS = 4
BLOCK = 128
UP_CHUNKS = 2
DOWN_CHUNKS = 4
ACTIVE = 3

BF16 = jnp.bfloat16
F32 = jnp.float32


def make_per_device(n_grp, n_fs, n_tp):
    ring = [(i, (i + 1) % n_fs) for i in range(n_fs)]
    swap = [(i, (i + 1) % n_grp) for i in range(n_grp)]

    def to_peer(value, offset):
        return lax.ppermute(value, "tp", [(i, i ^ offset) for i in range(n_tp)])

    def per_device(
        tokens,
        norm1_gain,
        weight_u,
        weight_v,
        scale_u,
        scale_v,
        mix_gain,
        spatial_weight,
        spatial_bias,
        weight_out,
        scale_out,
        norm2_gain,
        weight_up,
        scale_up,
        weight_down,
        scale_down,
    ):
        feature_count = norm1_gain.shape[0]
        token_count, width = tokens.shape
        grp_at = lax.axis_index("grp")
        fs_at = lax.axis_index("fs")
        tp_at = lax.axis_index("tp")

        def place_of(offset):
            return offset // 2 + (offset % 2) * (n_tp // 2)

        order = [r for r in range(n_tp) if r % 2 == 0] + [r for r in range(n_tp) if r % 2 == 1]

        def row_part(array, at):
            rows = array.shape[0] // n_grp
            return lax.dynamic_slice_in_dim(array, at * rows, rows, 0)

        class Chunk:
            def __init__(self, full):
                self.full = full
                self.last = row_part(full, grp_at)
                self.steps = []

        issued = []

        def issue(chunk):
            value = chunk.last
            if len(issued) >= ACTIVE:
                value, _ = lax.optimization_barrier((value, issued[-ACTIVE]))
            moved = lax.ppermute(value, "fs", ring)
            issued.append(moved)
            chunk.last = moved
            parts = [(0, moved)]
            other = moved
            for step in range(1, n_grp):
                other = lax.ppermute(other, "grp", swap)
                parts.append((step, other))
            chunk.steps.append(parts)

        def pieces(chunk):
            yield fs_at, 0, chunk.full
            rows = chunk.full.shape[0] // n_grp
            for step, parts in enumerate(chunk.steps, 1):
                for turn, value in parts:
                    yield (fs_at - step) % n_fs, ((grp_at - turn) % n_grp) * rows, value

        def row_gain(gain, rows):
            return lax.dynamic_slice_in_dim(gain, fs_at * rows, rows, 0)[:, None]

        def rounded(weight, factor):
            return (weight.astype(BF16).astype(F32) * factor).astype(BF16)

        uv_shard = jnp.concatenate(
            [
                rounded(weight_u, row_gain(norm1_gain, weight_u.shape[0])),
                rounded(weight_v, row_gain(norm1_gain, weight_v.shape[0])),
            ],
            axis=1,
        )
        out_shard = rounded(weight_out, scale_out[None, :])
        up_shard = rounded(weight_up, row_gain(norm2_gain, weight_up.shape[0]))
        down_shard = rounded(weight_down, scale_down[None, :])
        uv_chunk = Chunk(uv_shard)
        out_chunk = Chunk(out_shard)
        up_width = up_shard.shape[1] // UP_CHUNKS
        down_width = down_shard.shape[1] // DOWN_CHUNKS
        up_chunks = [
            Chunk(up_shard[:, c * up_width : (c + 1) * up_width]) for c in range(UP_CHUNKS)
        ]
        down_chunks = [
            Chunk(down_shard[:, c * down_width : (c + 1) * down_width]) for c in range(DOWN_CHUNKS)
        ]

        def gather_pieces(own):
            found = {0: own}
            for offset in range(2, n_tp, 2):
                found[offset] = to_peer(own, offset)
            for offset in range(0, n_tp, 2):
                found[offset + 1] = to_peer(found[offset], 1)
            return [found[offset] for offset in order]

        in_pieces = gather_pieces(tokens)

        waiting = [uv_chunk, out_chunk] + up_chunks + down_chunks
        active = []
        while waiting or active:
            while waiting and len(active) < ACTIVE:
                active.append(waiting.pop(0))
            for chunk in active:
                issue(chunk)
            active = [chunk for chunk in active if len(chunk.steps) < n_fs - 1]

        def feature_rows(chunk):
            rows = chunk.full.shape[0]
            whole = jnp.zeros((feature_count, chunk.full.shape[1]), BF16)
            for at, shift, value in pieces(chunk):
                first = at * rows
                owner = first // width
                start = place_of(owner ^ tp_at) * width + first - owner * width + shift
                whole = lax.dynamic_update_slice(whole, value, (start, 0))
            return whole

        per_owner = n_fs // n_tp

        def feature_columns(chunk):
            rows, columns = chunk.full.shape
            whole = jnp.zeros((rows, columns * n_fs), BF16)
            for at, shift, value in pieces(chunk):
                start = (place_of((at // per_owner) ^ tp_at) * per_owner + at % per_owner) * columns
                whole = lax.dynamic_update_slice(whole, value, (shift, start))
            return whole

        def scatter_product(left, whole):
            half = whole.shape[1] // 2
            piece = whole.shape[1] // n_tp
            theirs = jnp.dot(left, whole[:, half:], preferred_element_type=F32).astype(BF16)
            received = to_peer(theirs, 1)
            mine = jnp.dot(left, whole[:, :half], preferred_element_type=F32)
            mine = mine + received.astype(F32)
            total = mine[:, :piece]
            for at in range(1, n_tp // 2):
                part = mine[:, at * piece : (at + 1) * piece].astype(BF16)
                total = total + to_peer(part, 2 * at).astype(F32)
            return total

        widened_in = tokens.astype(F32)
        squares_in = lax.psum(jnp.sum(widened_in * widened_in, axis=1), "tp")
        inverse_in = lax.rsqrt(squares_in / feature_count + 1e-06)[:, None]
        pre = (
            jnp.dot(
                jnp.concatenate(in_pieces, axis=1),
                feature_rows(uv_chunk),
                preferred_element_type=F32,
            )
            * inverse_in
        )
        local_width = weight_u.shape[1]
        gate_u = jax.nn.gelu(pre[:, :local_width] * scale_u)
        act_v = jax.nn.gelu(pre[:, local_width:] * scale_v)
        row_sums, row_squares = lax.psum(
            (jnp.sum(act_v, axis=1), jnp.sum(act_v * act_v, axis=1)), "tp"
        )
        row_mean = (row_sums / GM_W)[:, None]
        square = (row_squares / GM_W)[:, None]
        v_norm = (
            (act_v - row_mean) * lax.rsqrt(square - row_mean * row_mean + 1e-06) * mix_gain
        ).astype(BF16)
        group_index = tp_at * local_width // (GM_W // GROUPS)
        lower_mask = jnp.tril(jnp.ones((BLOCK, BLOCK), F32))
        spatial_mask = (
            lax.dynamic_index_in_dim(spatial_weight, group_index, 0, keepdims=False) * lower_mask
        ).astype(BF16)
        block_bias = lax.dynamic_index_in_dim(spatial_bias, group_index, 0, keepdims=False)
        blocks = v_norm.reshape(-1, BLOCK, local_width)
        mixed_cols = jnp.einsum("ts,nsc->ntc", spatial_mask, blocks, preferred_element_type=F32)
        mixed_cols = mixed_cols + block_bias[None, :, None]
        gated = (gate_u * mixed_cols.reshape(-1, local_width)).astype(BF16)
        mixer_sum = scatter_product(gated, feature_columns(out_chunk))
        residual = (widened_in + mixer_sum).astype(BF16)

        mid_pieces = gather_pieces(residual)
        widened_mid = residual.astype(F32)
        squares_mid = lax.psum(jnp.sum(widened_mid * widened_mid, axis=1), "tp")
        inverse_mid = lax.rsqrt(squares_mid / feature_count + 1e-06)[:, None]
        full_up = jnp.concatenate([feature_rows(chunk) for chunk in up_chunks], axis=1)
        pre_up = (
            jnp.dot(jnp.concatenate(mid_pieces, axis=1), full_up, preferred_element_type=F32)
            * inverse_mid
        )
        hidden = jnp.square(jax.nn.relu(pre_up * scale_up)).astype(BF16)
        sums = [
            scatter_product(hidden, feature_columns(chunk)).reshape(
                token_count, per_owner, down_width
            )
            for chunk in down_chunks
        ]
        channel_sum = jnp.stack(sums, axis=2).reshape(token_count, width)
        return (widened_mid + channel_sum).astype(BF16)

    return per_device


def solution(mesh):
    placed = (
        P(("grp", "fs"), "tp"),
        P(),
        P("fs", "tp"),
        P("fs", "tp"),
        P("tp"),
        P("tp"),
        P("tp"),
        P(),
        P(),
        P("tp", "fs"),
        P("fs"),
        P(),
        P("fs", "tp"),
        P("tp"),
        P("tp", "fs"),
        P("fs"),
    )
    sizes = [mesh.shape[name] for name in ("grp", "fs", "tp")]
    return jax.shard_map(
        make_per_device(*sizes),
        mesh=mesh,
        in_specs=placed,
        out_specs=P(("grp", "fs"), "tp"),
        check_vma=False,
    )
```
